32 devices in a mesh: sp: 8 (over z, y), tp: 4 (over x, core).
Axes of the slice: x: 2, y: 2, z: 4, core: 2. Of those that a mesh axis runs over, the one named last changes fastest.
Arguments:
- residual: bfloat16 [2048, 2048], P(('sp', 'tp')), may hold values from -6 to 6
- receptance: bfloat16 [2048, 768], P('sp', 'tp'), may hold values from -6 to 6
- key_matrix: bfloat16 [2048, 768], P('sp', 'tp'), may hold values from -6 to 6
- values: bfloat16 [2048, 768], P('sp', 'tp'), may hold values from -6 to 6
- decay_dependent_logit: bfloat16 [2048, 768], P('sp', 'tp'), may hold values from -3.5 to 3.5
- decay_channel_offset: float32 [768], P('tp'), may hold values from -12.5 to -2.4
- extra_log_decay: float32 [2048, 768], P('sp', 'tp'), may hold values from -2.1 to 0
- removal_dependent_logit: bfloat16 [2048, 768], P('sp', 'tp'), may hold values from -4 to 4
- removal_channel_offset: float32 [768], P('tp'), may hold values from -8.1 to 0.5
- head_norm_gain: float32 [768], P('tp'), may hold values from 0.1 to 1.9
- output_matrix: bfloat16 [768, 2048], replicated, may hold values from -0.21875 to 0.21875
- expert_norm_gain: float32 [2048], replicated, may hold values from 0.1 to 1.9
- token_expert_index: int32 [2048, 2], P(('sp', 'tp')), may hold values from 0 to 7, all different within a row; in each aligned block of 64 rows (0 to 63, 64 to 127, ...) at most 32 rows name the same one
- token_expert_weight: float32 [2048, 2], P(('sp', 'tp')), may hold values from 0.2 to 1
- expert_gate_weight: bfloat16 [8, 2048, 3584], P('sp', None, 'tp'), may hold values from -0.125 to 0.125
- expert_up_weight: bfloat16 [8, 2048, 3584], P('sp', None, 'tp'), may hold values from -0.125 to 0.125
- expert_down_weight: bfloat16 [8, 3584, 2048], P('sp', 'tp'), may hold values from -0.09375 to 0.09375
Outputs:
- output: bfloat16 [2048, 2048], P(('sp', 'tp'))
The draws below stay inside these ranges and needn't reach their ends.
Inputs may be any that keep to these rules, and one draw needn't show every extreme that they name: `token_expert_index`: each row names 2 different experts. In each aligned block of 64 rows no expert is named by more than 32 rows, and in every draw some expert is named by exactly 32 rows of some block.
All inputs are finite; a program needn't handle non-finite values.
Results may differ from the reference program's by a relative error of at most 0.015.
Values may be sent and summed in bfloat16 or wider, within the bound.
A program may use at most 128 MiB of HBM per device.

```python
import math
import jax
import jax.numpy as jnp
import numpy as np
from jax import lax

D = 2048
HEADS = 12
HEAD = 64
RW = 768
FF = 3584
TOP = 2
TOK_DEV = 256
TOKENS = 2048
ROWS_DEV = 64
EXPERTS = 8
CAP = 32
N_SP = 8
N_TP = 4


def head_speed(key, share):
    pick = jax.random.uniform(jax.random.fold_in(key, 5), (HEADS,), jnp.float32)
    return jnp.repeat((pick < share).astype(jnp.float32), HEAD)


def draw_decay_channel_offset(key, part):
    fast = head_speed(key, 0.5)
    jitter = jax.random.uniform(jax.random.fold_in(key, 6), (HEADS * HEAD,), jnp.float32, -0.5, 0.5)
    slow_level = -jnp.log(jnp.float32(TOKENS)) - 1.5
    return fast * -2.9 + (1.0 - fast) * slow_level + jitter


def draw_removal_channel_offset(key, part):
    fast = head_speed(key, 0.5)
    jitter = jax.random.uniform(jax.random.fold_in(key, 8), (HEADS * HEAD,), jnp.float32, -0.5, 0.5)
    slow_level = jnp.log(jnp.float32(HEAD) / jnp.float32(TOKENS)) - 2.0
    return (1.0 - fast) * slow_level + jitter


def draw_decay_dependent_logit(key, part):
    noise = jnp.clip(jax.random.normal(jax.random.fold_in(key, 1), (TOKENS, HEADS * HEAD), jnp.float32), -4.0, 4.0) * 0.7
    offset = jax.random.uniform(jax.random.fold_in(key, 2), (TOKENS // TOK_DEV, 1, 1), jnp.float32, -0.7, 0.7)
    shaped = noise.reshape(TOKENS // TOK_DEV, TOK_DEV, HEADS * HEAD) + offset
    return shaped.reshape(TOKENS, HEADS * HEAD).astype(jnp.bfloat16)


def draw_extra_log_decay(key, part):
    spots = jax.random.randint(jax.random.fold_in(key, 3), (3,), 0, TOKENS)
    kept = jax.random.uniform(jax.random.fold_in(key, 4), (3, HEADS * HEAD), jnp.float32, 0.5, 0.8)
    hits = (jnp.arange(TOKENS)[:, None] == spots[None, :]).astype(jnp.float32)
    return jnp.dot(hits, jnp.log(kept), precision=lax.Precision.HIGHEST)


def level_of(own_key, dims, pieces, low, largest):
    level, own = 1.0, jax.random.fold_in(own_key, 6)
    for axis_at, blocks in pieces:
        steps = jnp.exp(jax.random.uniform(jax.random.fold_in(own, axis_at), (blocks,), jnp.float32, low / len(pieces), largest / len(pieces)))
        level = level * jnp.repeat(steps, dims[axis_at] // blocks).reshape([-1 if axis == axis_at else 1 for axis in range(len(dims))])
    return level


def routed_block(key, own, number, rows, amount, top, bound, slope):
    ranking = jax.random.permutation(key, amount)
    packed, ordinary = portions_of(amount, rows * top, bound, slope, True), portions_of(amount, rows * top, bound, slope, False)
    places = jnp.arange(amount)

    def named(lengths, offset_by):
        used = int((lengths > 0).sum())
        fixed = max(1, used // 4)
        shifted = fixed + (places - fixed + offset_by * (used - fixed)) % max(1, amount - fixed)
        return jnp.zeros((amount,), jnp.int32).at[ranking[jnp.where(places < fixed, places, shifted)]].set(jnp.asarray(lengths, jnp.int32))

    lengths = jnp.where(number % 4 == 0, named(packed, number // 4), named(ordinary, number - number // 4 - 1))
    mixed = jax.random.permutation(jax.random.fold_in(own, 3), amount)
    source_of, receiver = mixed[0:amount // 2 * 2:2], mixed[1:amount // 2 * 2:2]
    margin = jnp.minimum(lengths[source_of] - 1, bound - lengths[receiver]) // 2
    margin = jnp.where((source_of == ranking[0]) | (receiver == ranking[0]) | (lengths[receiver] == 0), 0, jnp.maximum(margin, 0))
    shifted = jax.random.randint(jax.random.fold_in(own, 4), (amount // 2,), 0, 1 << 20) % (margin + 1)
    lengths = lengths.at[source_of].add(-shifted).at[receiver].add(shifted)
    labels = jnp.searchsorted(jnp.cumsum(lengths), jnp.arange(rows * top), side="right").astype(jnp.int32)
    grid = labels.reshape(top, rows).T
    grid = grid[jax.random.permutation(jax.random.fold_in(own, 1), rows)]
    offset_by = jax.random.randint(jax.random.fold_in(own, 2), (rows, 1), 0, top)
    return jnp.take_along_axis(grid, (jnp.arange(top)[None, :] + offset_by) % top, axis=1)


def portions_of(count, total, bound, slope, full):
    portions = [(1 << 20) // math.isqrt(rank ** slope) + 1 for rank in range(1, count + 1)]
    largest = bound if full else min(bound, max(-(-total // count), total * portions[0] // sum(portions)))
    least = 1 if total - largest >= count - 1 else 0
    given, surplus = [largest] + [least] * (count - 1), total - largest - least * (count - 1)
    while surplus > 0:
        free = [i for i in range(1, count) if given[i] < largest] or [i for i in range(1, count) if given[i] < bound]
        pool, left = sum([portions[i] for i in free]), surplus
        for i in free:
            extra = min(bound - given[i], max(1, left * portions[i] // pool), surplus)
            given[i] = given[i] + extra
            surplus = surplus - extra
    return np.array(given)


def centred(stream_key, shape, scale, bound, pieces=(), kind=jnp.bfloat16):
    result = scale * jax.random.normal(stream_key, shape, jnp.float32)
    if pieces:
        result = result * level_of(stream_key, shape, pieces, -0.22, 0.18)
    return jnp.clip(result, -bound, bound).astype(kind)


def setup_inputs(seed: int = 0) -> dict:
    key_of = jax.random.split(jax.random.key(seed), 18)
    residual = centred(key_of[0], (TOKENS, D), 1.0, 6.0, ((0, 32),))
    receptance = centred(key_of[1], (TOKENS, RW), 1.0, 6.0, ((0, 8), (1, 4)))
    key_matrix = centred(key_of[2], (TOKENS, RW), 1.0, 6.0, ((0, 8), (1, 4)))
    values = centred(key_of[3], (TOKENS, RW), 1.0, 6.0, ((0, 8), (1, 4)))
    decay_dependent_logit = draw_decay_dependent_logit(jax.random.fold_in(key_of[17], 71), 0)
    decay_channel_offset = draw_decay_channel_offset(jax.random.fold_in(key_of[17], 71), 0)
    extra_log_decay = draw_extra_log_decay(jax.random.fold_in(key_of[17], 71), 0)
    removal_dependent_logit = centred(key_of[7], (TOKENS, RW), 1.0, 4.0, ((0, 8), (1, 4)))
    removal_channel_offset = draw_removal_channel_offset(jax.random.fold_in(key_of[17], 71), 0)
    head_norm_gain = jnp.clip(1.0 + 0.18 * jax.random.normal(key_of[9], (RW,), jnp.float32), 0.1, 1.9)
    output_matrix = centred(key_of[10], (RW, D), RW ** -0.5, 0.21875)
    expert_norm_gain = jnp.clip(1.0 + 0.18 * jax.random.normal(key_of[11], (D,), jnp.float32), 0.1, 1.9)
    token_expert_index_keys = jax.random.split(jax.random.fold_in(key_of[12], 1), TOKENS // ROWS_DEV)
    token_expert_index_turns = jax.random.permutation(jax.random.fold_in(key_of[12], 3), TOKENS // ROWS_DEV)
    token_expert_index = jax.vmap(lambda own, number: routed_block(jax.random.fold_in(key_of[12], 2), own, number, ROWS_DEV, EXPERTS, TOP, CAP, 2))(token_expert_index_keys, token_expert_index_turns).reshape((TOKENS, TOP))
    token_expert_weight = jnp.clip(0.2 + 0.8 * jax.random.uniform(key_of[13], (TOKENS, TOP), jnp.float32) ** level_of(key_of[13], (TOKENS, TOP), ((0, 32),), -0.2, 0.2), 0.2, 1.0)
    expert_gate_weight = centred(key_of[14], (EXPERTS, D, FF), D ** -0.5, 0.125, ((0, 8), (2, 4)))
    expert_up_weight = centred(key_of[15], (EXPERTS, D, FF), D ** -0.5, 0.125, ((0, 8), (2, 4)))
    expert_down_weight = centred(key_of[16], (EXPERTS, FF, D), FF ** -0.5, 0.09375, ((0, 8), (1, 4)))
    return {"residual": residual, "receptance": receptance, "key_matrix": key_matrix, "values": values, "decay_dependent_logit": decay_dependent_logit, "decay_channel_offset": decay_channel_offset, "extra_log_decay": extra_log_decay, "removal_dependent_logit": removal_dependent_logit, "removal_channel_offset": removal_channel_offset, "head_norm_gain": head_norm_gain, "output_matrix": output_matrix, "expert_norm_gain": expert_norm_gain, "token_expert_index": token_expert_index, "token_expert_weight": token_expert_weight, "expert_gate_weight": expert_gate_weight, "expert_up_weight": expert_up_weight, "expert_down_weight": expert_down_weight}


group_epsilon = 0.00064
norm_epsilon = 1e-06
unit_epsilon = 1e-06
highest = lax.Precision.HIGHEST

def log_decay_series(decay_dependent_logit, decay_channel_offset, extra_log_decay):
    current_tier = decay_channel_offset[None, :] + decay_dependent_logit.astype(jnp.float32)
    return -jnp.exp(-jax.nn.softplus(-current_tier) - 0.5) + extra_log_decay

def learn_rates(removal_dependent_logit, removal_channel_offset):
    return jax.nn.sigmoid(removal_channel_offset[None, :] + removal_dependent_logit.astype(jnp.float32))

def unit_rows(key_heads):
    return key_heads * lax.rsqrt(lax.optimization_barrier(jnp.sum(key_heads * key_heads, axis=-1, keepdims=True)) + unit_epsilon)

def group_norm(heads_out, head_norm_gain):
    center = heads_out - lax.optimization_barrier(jnp.mean(heads_out, axis=-1, keepdims=True))
    spread = lax.optimization_barrier(jnp.mean(center * center, axis=-1, keepdims=True))
    scaled = center * lax.rsqrt(spread + group_epsilon)
    return (scaled.reshape(scaled.shape[0], -1) * head_norm_gain[None, :]).astype(jnp.bfloat16)

def split_heads(array):
    return array.astype(jnp.float32).reshape(array.shape[0], HEADS, HEAD)

def recurrence(receptance, key_matrix, values, log_decay_value, rates):
    read_heads = split_heads(receptance)
    key_heads = split_heads(key_matrix)
    value_heads = split_heads(values)
    decay_heads = jnp.exp(split_heads(log_decay_value))
    rate_heads = split_heads(rates)
    unit_heads = unit_rows(key_heads)

    def advance(memory, inputs):
        read_now, decay_now, key_now, value_now, unit_now, rate_now = inputs
        removed = jnp.einsum('hvk,hk->hv', memory, unit_now, precision=highest)
        memory = memory * decay_now[:, None, :] - removed[:, :, None] * (unit_now * rate_now)[:, None, :] + value_now[:, :, None] * key_now[:, None, :]
        return (memory, jnp.einsum('hvk,hk->hv', memory, read_now, precision=highest))
    initial = jnp.zeros((HEADS, HEAD, HEAD), jnp.float32)
    _, outputs = lax.scan(advance, initial, (read_heads, decay_heads, key_heads, value_heads, unit_heads, rate_heads))
    return outputs

def reference(residual, receptance, key_matrix, values, decay_dependent_logit, decay_channel_offset, extra_log_decay, removal_dependent_logit, removal_channel_offset, head_norm_gain, output_matrix, expert_norm_gain, token_expert_index, token_expert_weight, expert_gate_weight, expert_up_weight, expert_down_weight):
    log_decay_value = log_decay_series(decay_dependent_logit, decay_channel_offset, extra_log_decay)
    rates = learn_rates(removal_dependent_logit, removal_channel_offset)
    heads_out = recurrence(receptance, key_matrix, values, log_decay_value, rates)
    mixed = group_norm(heads_out, head_norm_gain)
    after_mix = residual.astype(jnp.float32) + jnp.dot(mixed, output_matrix, preferred_element_type=jnp.float32)
    normed = (after_mix * lax.rsqrt(lax.optimization_barrier(jnp.mean(after_mix * after_mix, axis=-1, keepdims=True)) + norm_epsilon) * expert_norm_gain[None, :]).astype(jnp.bfloat16)
    devices = N_SP * N_TP
    rows_dev = TOKENS // devices
    flat_ids = token_expert_index.reshape(devices, rows_dev * TOP)
    onehot = (flat_ids[:, :, None] == jnp.arange(EXPERTS, dtype=jnp.int32)[None, None, :]).astype(jnp.int32)
    slot_rank = lax.optimization_barrier(jnp.sum((jnp.cumsum(onehot, axis=1) - onehot) * onehot, axis=-1))
    per_expert = devices * CAP
    slot_index = (flat_ids * per_expert + jnp.arange(devices, dtype=jnp.int32)[:, None] * CAP + slot_rank).reshape(-1)
    token_index = jnp.arange(TOKENS * TOP, dtype=jnp.int32) // TOP
    row_table = jnp.full((EXPERTS * per_expert,), TOKENS, jnp.int32).at[slot_index].set(token_index)
    padded = jnp.concatenate([normed, jnp.zeros((1, D), jnp.bfloat16)], axis=0)
    group_width = FF // N_TP

    def run_expert(operands):
        row_ids, gate_weight, up_weight, down_weight = operands
        routed = padded[row_ids]
        gate_out = jnp.dot(routed, gate_weight, preferred_element_type=jnp.float32)
        up_out = jnp.dot(routed, up_weight, preferred_element_type=jnp.float32)
        hidden = (jax.nn.silu(gate_out) * up_out).astype(jnp.bfloat16)
        summed = jnp.zeros((routed.shape[0], D), jnp.float32)
        for quarter in range(N_TP):
            partial_sum = jnp.dot(hidden[:, quarter * group_width:(quarter + 1) * group_width], down_weight[quarter * group_width:(quarter + 1) * group_width], preferred_element_type=jnp.float32).astype(jnp.bfloat16)
            summed = summed + lax.optimization_barrier(partial_sum).astype(jnp.float32)
        return summed.astype(jnp.bfloat16)
    returned = lax.map(run_expert, (row_table.reshape(EXPERTS, per_expert), expert_gate_weight, expert_up_weight, expert_down_weight))
    picked = returned.reshape(EXPERTS * per_expert, D)[slot_index].reshape(TOKENS, TOP, D)
    routed_sum = lax.optimization_barrier(jnp.sum(token_expert_weight[:, :, None] * picked.astype(jnp.float32), axis=1))
    return (after_mix + routed_sum).astype(jnp.bfloat16)
```

```python
import functools

import jax
import jax.numpy as jnp
from jax import lax
from jax.experimental import pallas as pl
from jax.experimental.pallas import tpu as pltpu
from jax.sharding import PartitionSpec as P

HEAD = 64
CHUNK = 32
MESH = pl.DeviceIdType.MESH

group_epsilon = 0.00064
norm_epsilon = 1e-06
unit_epsilon = 1e-06

f32 = jnp.float32
bf16 = jnp.bfloat16
NN = (((1,), (0,)), ((), ()))
NT = (((1,), (1,)), ((), ()))


def dot1(a, b, dims=NN):
    return lax.dot_general(a, b, dims, preferred_element_type=f32)


def parts(a):
    high = a.astype(bf16)
    return high, (a - high.astype(f32)).astype(bf16)


def dot3(a, b, dims=NN):
    ah, al = parts(a)
    bh, bl = parts(b)
    return dot1(ah, bh, dims) + (dot1(ah, bl, dims) + dot1(al, bh, dims))


def meet(groups):
    barrier = pltpu.get_barrier_semaphore()
    for device in groups:
        pl.semaphore_signal(barrier, inc=1, device_id=device, device_id_type=MESH)
    pl.semaphore_wait(barrier, len(groups))


def remote(src, dst, send, recv, device):
    return pltpu.make_async_remote_copy(
        src_ref=src, dst_ref=dst, send_sem=send, recv_sem=recv, device_id=device, device_id_type=MESH
    )


def token_slots(index, experts, cap):
    rows, top = index.shape
    lane = lax.broadcasted_iota(jnp.int32, (rows, 128), 1)
    named = [(index[:, k : k + 1] == lane).astype(f32) for k in range(top)]
    row = lax.broadcasted_iota(jnp.int32, (rows, rows), 0)
    col = lax.broadcasted_iota(jnp.int32, (rows, rows), 1)
    before = dot1((row > col).astype(bf16), sum(named).astype(bf16))
    slots = []
    for k in range(top):
        rank = jnp.sum(before * named[k], axis=1, keepdims=True)
        slots.append(index[:, k : k + 1].astype(f32) * cap + rank)
        before = before + named[k]
    return slots


def mixer_kernel(
    n_sp,
    n_tp,
    cap,
    residual,
    receptance,
    key_matrix,
    values,
    decay_logit,
    decay_offset,
    extra,
    rate_logit,
    rate_offset,
    gain,
    out_matrix,
    norm_gain,
    index,
    after_mix,
    outgoing,
    matrix_vmem,
    pair_out,
    pair_in,
    mixed_out,
    mixed_in,
    matrix_sem,
    pair_send,
    pair_recv,
    mixed_send,
    mixed_recv,
):
    s, t = lax.axis_index("sp"), lax.axis_index("tp")
    load = pltpu.make_async_copy(out_matrix, matrix_vmem, matrix_sem)
    load.start()
    meet(
        [(lax.rem(s + k, n_sp), t) for k in range(1, n_sp)]
        + [(s, lax.rem(t + k, n_tp)) for k in range(1, n_tp)]
    )
    tokens, width = receptance.shape
    heads = width // HEAD
    chunks = tokens // CHUNK
    row = lax.broadcasted_iota(jnp.int32, (tokens, tokens), 0)
    col = lax.broadcasted_iota(jnp.int32, (tokens, tokens), 1)
    together = row // CHUNK == col // CHUNK
    middle = row // CHUNK * CHUNK + CHUNK // 2 - 1
    lower = together & (row >= col)
    strict = together & (row > col)
    reach = (together & (col <= middle)).astype(f32)
    logd = -jnp.exp(-jax.nn.softplus(-(decay_offset[...] + decay_logit[...].astype(f32))) - 0.5)
    logd = logd + extra[...]
    rates = jax.nn.sigmoid(rate_offset[...] + rate_logit[...].astype(f32))
    d0 = logd.astype(bf16)
    rest = logd - d0.astype(f32)
    d1 = rest.astype(bf16)
    d2 = (rest - d1.astype(f32)).astype(bf16)
    span = (lower.astype(f32) - reach).astype(bf16)
    whole = together.astype(bf16)
    reach = reach.astype(bf16)

    def total(mask):
        return dot1(mask, d0) + (dot1(mask, d1) + dot1(mask, d2))

    relative = total(span)
    to_middle = total(reach)
    chunk_sum = total(whole)
    to_end = jnp.exp(chunk_sum - to_middle - relative)
    grow = jnp.exp(-relative)
    shrink = jnp.exp(relative)
    shrink_before = jnp.exp(relative - logd)
    entry = jnp.exp(to_middle)
    chunk_decay = jnp.exp(chunk_sum)

    keys = key_matrix[...].astype(f32)
    read = receptance[...].astype(f32)
    value = values[...].astype(f32)
    each = range(heads)

    def head(a, h):
        return a[:, h * HEAD : (h + 1) * HEAD]

    key_h = [head(keys, h) for h in each]
    val_h = [head(value, h) for h in each]
    unit = [
        a * lax.rsqrt(jnp.sum(a * a, axis=1, keepdims=True) + unit_epsilon) for a in key_h
    ]
    write = [unit[h] * head(rates, h) for h in each]
    remove = [-unit[h] * head(shrink_before, h) for h in each]
    reading = [head(read, h) * head(shrink, h) for h in each]
    gram = [
        dot3(
            jnp.concatenate([remove[h], reading[h]], axis=0),
            jnp.concatenate([write[h] * head(grow, h), key_h[h] * head(grow, h)], axis=0),
            NT,
        )
        for h in each
    ]
    couple_write = [jnp.where(strict, g[:tokens, :tokens], 0.0) for g in gram]
    couple_key = [jnp.where(strict, g[:tokens, tokens:], 0.0) for g in gram]
    read_write = [jnp.where(lower, g[tokens:, :tokens], 0.0) for g in gram]
    read_key = [jnp.where(lower, g[tokens:, tokens:], 0.0) for g in gram]
    inverse = [
        (row == col).astype(f32) + jnp.where(row // 2 == col // 2, c, 0.0) for c in couple_write
    ]
    size = 4
    while size <= CHUNK:
        joined = (row // size == col // size) & (row // (size // 2) != col // (size // 2))
        half = [dot3(jnp.where(joined, couple_write[h], 0.0), inverse[h]) for h in each]
        inverse = [inverse[h] + dot3(inverse[h], half[h]) for h in each]
        size *= 2
    seen = [dot3(jnp.concatenate([couple_key[h], read_key[h]], axis=0), val_h[h]) for h in each]
    solved = [
        dot3(inverse[h], jnp.concatenate([remove[h], seen[h][:tokens]], axis=1)) for h in each
    ]
    answer = [dot3(read_write[h], solved[h]) for h in each]
    readout = [(reading[h] + answer[h][:, :HEAD]) * head(entry, h) for h in each]
    local = [answer[h][:, HEAD:] + seen[h][tokens:] for h in each]
    lane_chunk = lax.broadcasted_iota(jnp.int32, (tokens, chunks * HEAD), 1) // HEAD
    row_chunk = lax.broadcasted_iota(jnp.int32, (tokens, chunks * HEAD), 0) // CHUNK
    own_chunk = lane_chunk == row_chunk
    steps = []
    for h in each:
        scaled = jnp.concatenate([solved[h][:, :HEAD] * head(entry, h), solved[h][:, HEAD:]], axis=1)
        write_end = write[h] * head(to_end, h)
        key_end = key_h[h] * head(to_end, h)
        spread_write = jnp.where(own_chunk, jnp.concatenate([write_end] * chunks, axis=1), 0.0)
        spread_key = jnp.where(own_chunk, jnp.concatenate([key_end] * chunks, axis=1), 0.0)
        held = jnp.concatenate([jnp.zeros_like(val_h[h]), val_h[h]], axis=1)
        steps.append(dot3(scaled.T, spread_write) + dot3(held.T, spread_key))
    prow = lax.broadcasted_iota(jnp.int32, (2 * HEAD, HEAD), 0)
    pcol = lax.broadcasted_iota(jnp.int32, (2 * HEAD, HEAD), 1)
    pair = [(prow == pcol).astype(f32) for _ in each]
    before = [[] for _ in each]
    for c in range(chunks):
        for h in each:
            before[h].append(pair[h])
            step = steps[h][:, c * HEAD : (c + 1) * HEAD]
            decay = head(chunk_decay, h)[c * CHUNK : c * CHUNK + 1]
            moved = dot3(pair[h], step[:HEAD])
            added = jnp.concatenate([jnp.zeros((HEAD, HEAD), f32), step[HEAD:]], axis=0)
            pair[h] = pair[h] * decay + moved + added
    for h in each:
        pair_out[h * HEAD : (h + 1) * HEAD, :] = jnp.concatenate(
            [pair[h][:HEAD], pair[h][HEAD:]], axis=1
        ).astype(bf16)

    def pair_copy(to):
        return remote(pair_out, pair_in.at[s], pair_send.at[to], pair_recv.at[s], (to, t))

    for to in range(n_sp):

        @pl.when(to > s)
        def _():
            pair_copy(to).start()

    after = []
    for h in each:
        rows = [
            dot3(readout[h][c * CHUNK : (c + 1) * CHUNK], before[h][c], NT) for c in range(chunks)
        ]
        both = jnp.concatenate(rows, axis=0)
        after.append((both[:, :HEAD], both[:, HEAD:] + local[h]))
    slots = token_slots(index[...], n_sp, cap)

    def hop(origin, states):
        remote(
            pair_out, pair_in.at[origin], pair_send.at[0], pair_recv.at[origin], (origin, t)
        ).wait_recv()
        got = pair_in[origin]
        result = []
        for h in each:
            mine = got[h * HEAD : (h + 1) * HEAD]
            high, low = parts(states[h])
            moved = dot1(high, mine[:, :HEAD]) + dot1(low, mine[:, :HEAD])
            result.append(moved + mine[:, HEAD:].astype(f32))
        return tuple(result)

    states = lax.fori_loop(0, s, hop, tuple(jnp.zeros((HEAD, HEAD), f32) for _ in each))
    mixed = []
    for h in each:
        out = after[h][1] + dot3(after[h][0], states[h], NT)
        center = out - jnp.mean(out, axis=1, keepdims=True)
        spread = jnp.mean(center * center, axis=1, keepdims=True)
        mixed.append(center * lax.rsqrt(spread + group_epsilon))
    mixed = (jnp.concatenate(mixed, axis=1) * gain[...]).astype(bf16)
    share = tokens // n_tp
    for j in range(n_tp):
        mixed_out[j] = mixed[j * share : (j + 1) * share]
    mixed_copies = []
    for k in range(1, n_tp):
        to = lax.rem(t + k, n_tp)
        copy = remote(
            mixed_out.at[to], mixed_in.at[t], mixed_send.at[k], mixed_recv.at[t], (s, to)
        )
        copy.start()
        mixed_copies.append(copy)
    load.wait()
    total_mix = residual[...].astype(f32) + dot1(mixed_out[t], matrix_vmem[t])
    for k in range(1, n_tp):
        origin = lax.rem(t + n_tp - k, n_tp)
        remote(
            mixed_out.at[0], mixed_in.at[origin], mixed_send.at[k], mixed_recv.at[origin], (s, origin)
        ).wait_recv()
        total_mix = total_mix + dot1(mixed_in[origin], matrix_vmem[origin])
    after_mix[...] = total_mix
    scale = lax.rsqrt(jnp.mean(total_mix * total_mix, axis=1, keepdims=True) + norm_epsilon)
    normed = (total_mix * scale * norm_gain[...]).astype(bf16)
    slot_rows = [jnp.broadcast_to(a, (a.shape[0], 128)).T[:1] for a in slots]
    for e in range(n_sp):
        place = lax.broadcasted_iota(jnp.int32, (cap, normed.shape[0]), 0).astype(f32) + e * cap
        pick = sum((a == place).astype(f32) for a in slot_rows).astype(bf16)
        outgoing[e] = dot1(pick, normed).astype(bf16)
    for copy in mixed_copies:
        copy.wait_send()
    for to in range(n_sp):

        @pl.when(to > s)
        def _():
            pair_copy(to).wait_send()


def split_tp(n_tp):
    low = 2 if n_tp % 2 == 0 else 1
    return n_tp // low, low


def dispatch_kernel(n_sp, n_tp, outgoing, rows, own_sem, far_send, wide_send, near_send, recv):
    s, t = lax.axis_index("sp"), lax.axis_index("tp")
    n_high, n_low = split_tp(n_tp)
    high, low = t // n_low, lax.rem(t, n_low)
    meet(
        [(lax.rem(s + k, n_sp), t) for k in range(1, n_sp)]
        + [(s, lax.rem(high + k, n_high) * n_low + low) for k in range(1, n_high)]
        + [(s, high * n_low + lax.rem(low + k, n_low)) for k in range(1, n_low)]
    )
    sends = []

    def start(src, at, send, device):
        copy = remote(src, rows.at[at[0], at[1]], send, recv.at[at[0], at[1]], device)
        copy.start()
        sends.append(copy)

    for k in range(n_sp - 1, 0, -1):
        to = lax.rem(s + k, n_sp)
        start(outgoing.at[to], (s, t), far_send.at[k], (to, t))
    own = pltpu.make_async_copy(outgoing.at[s], rows.at[s, t], own_sem)
    own.start()

    def landed(origin, column):
        remote(
            rows.at[origin, column], rows.at[origin, column], own_sem, recv.at[origin, column], (s, t)
        ).wait_recv()

    def spread(src, origin, column, k):
        for j in range(1, n_low):
            peer = high * n_low + lax.rem(low + j, n_low)
            start(src, (origin, column), near_send.at[k, column // n_low, j], (s, peer))

    def widen(src, origin, k):
        for j in range(1, n_high):
            peer = lax.rem(high + j, n_high) * n_low + low
            start(src, (origin, t), wide_send.at[k, j], (s, peer))

    def relay(k):
        origin = lax.rem(s + k, n_sp)
        for j in range(1, n_high):
            column = lax.rem(high + j, n_high) * n_low + low
            landed(origin, column)
            spread(rows.at[origin, column], origin, column, k)

    widen(outgoing.at[s], s, 0)
    spread(outgoing.at[s], s, t, 0)
    for k in range(1, n_sp):
        origin = lax.rem(s + k, n_sp)
        landed(origin, t)
        widen(rows.at[origin, t], origin, k)
        spread(rows.at[origin, t], origin, t, k)
        relay(k - 1)
    relay(n_sp - 1)
    for k in range(n_sp):
        origin = lax.rem(s + k, n_sp)
        for j in range(1, n_low):
            for i in range(n_high):
                landed(origin, i * n_low + lax.rem(low + j, n_low))
    own.wait()
    for copy in sends:
        copy.wait_send()


def combine_kernel(
    n_sp,
    n_tp,
    partial,
    after_mix,
    index,
    weight,
    out,
    near_in,
    wide_out,
    wide_in,
    summed,
    returned,
    near_send,
    near_recv,
    wide_send,
    wide_recv,
    far_send,
    far_recv,
):
    s, t = lax.axis_index("sp"), lax.axis_index("tp")
    n_high, n_low = split_tp(n_tp)
    high, low = t // n_low, lax.rem(t, n_low)
    cap = partial.shape[2]
    meet(
        [(lax.rem(s + k, n_sp), t) for k in range(1, n_sp)]
        + [(s, lax.rem(high + k, n_high) * n_low + low) for k in range(1, n_high)]
        + [(s, high * n_low + lax.rem(low + k, n_low)) for k in range(1, n_low)]
    )
    sends = []

    def start(copy):
        copy.start()
        sends.append(copy)

    order = [k for k in range(n_sp - 1, -1, -1)]
    for k in order:
        q = lax.rem(s + k, n_sp)
        for i in list(range(1, n_high)) + [0]:
            row = lax.rem(high + i, n_high)
            for j in range(1, n_low):
                peer_low = lax.rem(low + j, n_low)
                start(
                    remote(
                        partial.at[q, row * n_low + peer_low],
                        near_in.at[k, i, j - 1],
                        near_send.at[k, i, j - 1],
                        near_recv.at[k, i, j - 1],
                        (s, high * n_low + peer_low),
                    )
                )

    def near_sum(k, i):
        q = lax.rem(s + k, n_sp)
        row = lax.rem(high + i, n_high)
        value = partial[q, row * n_low + low].astype(f32)
        for j in range(1, n_low):
            remote(
                near_in.at[k, i, j - 1],
                near_in.at[k, i, j - 1],
                near_send.at[k, i, j - 1],
                near_recv.at[k, i, j - 1],
                (s, t),
            ).wait_recv()
            value = value + near_in[k, i, j - 1].astype(f32)
        return value

    def send_wide(k):
        for i in range(1, n_high):
            to = lax.rem(high + i, n_high) * n_low + low
            start(
                remote(
                    wide_out.at[k, i - 1],
                    wide_in.at[k, i - 1],
                    wide_send.at[k, i - 1],
                    wide_recv.at[k, i - 1],
                    (s, to),
                )
            )

    for at, k in enumerate(order):
        for i in range(1, n_high):
            wide_out[k, i - 1] = near_sum(k, i).astype(bf16)
        if at:
            send_wide(order[at - 1])
    send_wide(order[-1])

    def send_far(k):
        if k:
            q = lax.rem(s + k, n_sp)
            start(remote(summed.at[k], returned.at[k], far_send.at[k], far_recv.at[k], (q, t)))

    for at, k in enumerate(order):
        value = near_sum(k, 0)
        for i in range(1, n_high):
            remote(
                wide_out.at[k, i - 1],
                wide_in.at[k, i - 1],
                wide_send.at[k, i - 1],
                wide_recv.at[k, i - 1],
                (s, t),
            ).wait_recv()
            value = value + wide_in[k, i - 1].astype(f32)
        summed[k] = value.astype(bf16)
        if at:
            send_far(order[at - 1])
    send_far(order[-1])

    slots = token_slots(index[...], n_sp, cap)
    rows = after_mix.shape[0]
    place = lax.broadcasted_iota(jnp.int32, (rows, cap), 1).astype(f32)
    total = after_mix[...]
    for k in range(n_sp):
        expert = lax.rem(s + n_sp - k, n_sp)
        if k:
            remote(
                summed.at[k], returned.at[k], far_send.at[k], far_recv.at[k], (expert, t)
            ).wait_recv()
        got = returned[k] if k else summed[0]
        base = (expert * cap).astype(f32)
        pick = sum(
            jnp.where(slots[j] == place + base, weight[:, j : j + 1], 0.0) for j in range(len(slots))
        )
        pick_high, pick_low = parts(pick)
        total = total + (dot1(pick_high, got) + dot1(pick_low, got))
    out[...] = total.astype(bf16)
    for copy in sends:
        copy.wait_send()


def expert_hidden(routed, gate_weight, up_weight):
    gate_out = jnp.dot(routed, gate_weight, preferred_element_type=jnp.float32)
    up_out = jnp.dot(routed, up_weight, preferred_element_type=jnp.float32)
    return (jax.nn.silu(gate_out) * up_out).astype(jnp.bfloat16)


VMEM = pl.BlockSpec(memory_space=pltpu.VMEM)
ANY = pl.BlockSpec(memory_space=pl.ANY)
DMA = pltpu.SemaphoreType.DMA


def params(number):
    return pltpu.CompilerParams(
        collective_id=number, has_side_effects=True, vmem_limit_bytes=60 * 1024 * 1024
    )


def body(
    n_sp,
    n_tp,
    residual,
    receptance,
    key_matrix,
    values,
    decay_dependent_logit,
    decay_channel_offset,
    extra_log_decay,
    removal_dependent_logit,
    removal_channel_offset,
    head_norm_gain,
    output_matrix,
    expert_norm_gain,
    token_expert_index,
    token_expert_weight,
    expert_gate_weight,
    expert_up_weight,
    expert_down_weight,
):
    rows_dev, width = residual.shape
    tokens, channels = receptance.shape
    top_count = token_expert_index.shape[1]
    cap = 2 * rows_dev * top_count // n_sp
    heads = channels // HEAD
    after_mix, outgoing = pl.pallas_call(
        functools.partial(mixer_kernel, n_sp, n_tp, cap),
        out_shape=(
            jax.ShapeDtypeStruct((rows_dev, width), f32),
            jax.ShapeDtypeStruct((n_sp, cap, width), bf16),
        ),
        in_specs=[VMEM] * 10 + [ANY] + [VMEM] * 2,
        out_specs=(VMEM, VMEM),
        scratch_shapes=[
            pltpu.VMEM((n_tp, channels, width), bf16),
            pltpu.VMEM((heads * HEAD, 2 * HEAD), bf16),
            pltpu.VMEM((n_sp, heads * HEAD, 2 * HEAD), bf16),
            pltpu.VMEM((n_tp, tokens // n_tp, channels), bf16),
            pltpu.VMEM((n_tp, tokens // n_tp, channels), bf16),
            DMA,
            DMA((n_sp,)),
            DMA((n_sp,)),
            DMA((n_tp,)),
            DMA((n_tp,)),
        ],
        compiler_params=params(0),
        name="mixer",
    )(
        residual,
        receptance,
        key_matrix,
        values,
        decay_dependent_logit,
        decay_channel_offset[None],
        extra_log_decay,
        removal_dependent_logit,
        removal_channel_offset[None],
        head_norm_gain[None],
        output_matrix.reshape(n_tp, channels, width),
        expert_norm_gain[None],
        token_expert_index,
    )
    n_high, n_low = split_tp(n_tp)
    rows = pl.pallas_call(
        functools.partial(dispatch_kernel, n_sp, n_tp),
        out_shape=jax.ShapeDtypeStruct((n_sp, n_tp, cap, width), bf16),
        in_specs=[VMEM],
        out_specs=ANY,
        scratch_shapes=[
            DMA,
            DMA((n_sp,)),
            DMA((n_sp, n_high)),
            DMA((n_sp, n_high, n_low)),
            DMA((n_sp, n_tp)),
        ],
        compiler_params=params(1),
        name="dispatch",
    )(outgoing)
    flat_rows = rows.reshape(-1, width)
    hidden = expert_hidden(flat_rows, expert_gate_weight[0], expert_up_weight[0])
    partial = jnp.dot(hidden, expert_down_weight[0], preferred_element_type=f32).astype(bf16)
    return pl.pallas_call(
        functools.partial(combine_kernel, n_sp, n_tp),
        out_shape=jax.ShapeDtypeStruct((rows_dev, width), bf16),
        in_specs=[VMEM] * 4,
        out_specs=VMEM,
        scratch_shapes=[
            pltpu.VMEM((n_sp, n_high, max(n_low - 1, 1), cap, width), bf16),
            pltpu.VMEM((n_sp, max(n_high - 1, 1), cap, width), bf16),
            pltpu.VMEM((n_sp, max(n_high - 1, 1), cap, width), bf16),
            pltpu.VMEM((n_sp, cap, width), bf16),
            pltpu.VMEM((n_sp, cap, width), bf16),
            DMA((n_sp, n_high, max(n_low - 1, 1))),
            DMA((n_sp, n_high, max(n_low - 1, 1))),
            DMA((n_sp, max(n_high - 1, 1))),
            DMA((n_sp, max(n_high - 1, 1))),
            DMA((n_sp,)),
            DMA((n_sp,)),
        ],
        compiler_params=params(2),
        name="combine",
    )(
        partial.reshape(n_sp, n_tp, cap, width),
        after_mix,
        token_expert_index,
        token_expert_weight,
    )


def solution(mesh):
    n_sp, n_tp = mesh.shape["sp"], mesh.shape["tp"]
    in_specs = (
        P(("sp", "tp"), None),
        P("sp", "tp"),
        P("sp", "tp"),
        P("sp", "tp"),
        P("sp", "tp"),
        P("tp"),
        P("sp", "tp"),
        P("sp", "tp"),
        P("tp"),
        P("tp"),
        P(),
        P(),
        P(("sp", "tp"), None),
        P(("sp", "tp"), None),
        P("sp", None, "tp"),
        P("sp", None, "tp"),
        P("sp", "tp", None),
    )
    out_specs = P(("sp", "tp"), None)
    return jax.shard_map(
        functools.partial(body, n_sp, n_tp),
        mesh=mesh,
        in_specs=in_specs,
        out_specs=out_specs,
        check_vma=False,
    )
```
